32 devices in a mesh: ep: 8 (over z, y), tp: 4 (over x, core).
Axes of the slice: x: 2, y: 2, z: 4, core: 2. Of those that a mesh axis runs over, the one named last changes fastest.
Arguments:
- c_gate: bfloat16 [2048, 1024], P('ep', 'tp'), may hold values from -6 to 6
- b_gate: bfloat16 [2048, 1024], P('ep', 'tp'), may hold values from -6 to 6
- values: bfloat16 [2048, 1024], P('ep', 'tp'), may hold values from -6 to 6
- conv_taps: float32 [3, 1024], P(None, 'tp'), may hold values from -3.5 to 3.5
- w_mix_out: bfloat16 [1024, 2048], P('tp'), may hold values from -0.1875 to 0.1875
- moe_in: bfloat16 [4096, 2048], P(('ep', 'tp')), may hold values from -6 to 6
- norm_gain: float32 [2048], replicated, may hold values from 0.1 to 1.9
- route_ids: int32 [4096, 2], P(('ep', 'tp')), may hold values from 0 to 7, all different within a row; in each aligned block of 128 rows (0 to 127, 128 to 255, ...) at most 40 rows name the same one
- route_weights: float32 [4096, 2], P(('ep', 'tp')), may hold values from 0.1 to 1
- w_gate: bfloat16 [8, 2048, 3584], P('ep', None, 'tp'), may hold values from -0.125 to 0.125
- w_up: bfloat16 [8, 2048, 3584], P('ep', None, 'tp'), may hold values from -0.125 to 0.125
- w_down: bfloat16 [8, 3584, 2048], P('ep', 'tp'), may hold values from -0.09375 to 0.09375
Outputs:
- mixer_out: bfloat16 [2048, 2048], P(('ep', 'tp'))
- moe_out: bfloat16 [4096, 2048], P(('ep', 'tp'))
The draws below stay inside these ranges and needn't reach their ends.
Inputs may be any that keep to these rules, and one draw needn't show every extreme that they name: `route_ids`: each row names 2 different experts; in each aligned block of 128 rows (the rows of one device) no expert is named by more than 40 rows, and in every draw some expert is named by exactly 40 rows in some block.
All inputs are finite; a program needn't handle non-finite values.
Results may differ from the reference program's by a relative error of at most 0.012.
Values may be sent and summed in bfloat16 or wider, within the bound.
A program may use at most 128 MiB of HBM per device.

```python
import math
import jax
import jax.numpy as jnp
import numpy as np
from jax import lax

D = 2048
WC = 1024
FF = 3584
KCONV = 3
TOP = 2
ROWS_B = 128
EXPERTS = 8
TOKA = 2048
TOKB = 4096
CAP = 40
SLOTS = 1280
N_EP = 8
N_TP = 4


def shard_levels(stream_key, shape, shards, smallest, largest):
    factor_of, own = 1.0, jax.random.fold_in(stream_key, 6)
    for axis_at, shards_of in shards:
        draws = jnp.exp(jax.random.uniform(jax.random.fold_in(own, axis_at), (shards_of,), jnp.float32, smallest / len(shards), largest / len(shards)))
        factor_of = factor_of * jnp.repeat(draws, shape[axis_at] // shards_of).reshape([-1 if axis == axis_at else 1 for axis in range(len(shape))])
    return factor_of


def shared_out(stream_key, own, number, rows, number_of, top, limit, lean):
    ranking = jax.random.permutation(stream_key, number_of)
    crowded, ordinary = shares(number_of, rows * top, limit, lean, True), shares(number_of, rows * top, limit, lean, False)
    places = jnp.arange(number_of)

    def named(lengths, offset_by):
        used = int((lengths > 0).sum())
        fixed = max(1, used // 4)
        passed = fixed + (places - fixed + offset_by * (used - fixed)) % max(1, number_of - fixed)
        return jnp.zeros((number_of,), jnp.int32).at[ranking[jnp.where(places < fixed, places, passed)]].set(jnp.asarray(lengths, jnp.int32))

    lengths = jnp.where(number % 4 == 0, named(crowded, number // 4), named(ordinary, number - number // 4 - 1))
    mixed = jax.random.permutation(jax.random.fold_in(own, 3), number_of)
    giver, sink = mixed[0:number_of // 2 * 2:2], mixed[1:number_of // 2 * 2:2]
    margin = jnp.minimum(lengths[giver] - 1, limit - lengths[sink]) // 2
    margin = jnp.where((giver == ranking[0]) | (sink == ranking[0]) | (lengths[sink] == 0), 0, jnp.maximum(margin, 0))
    passed = jax.random.randint(jax.random.fold_in(own, 4), (number_of // 2,), 0, 1 << 20) % (margin + 1)
    lengths = lengths.at[giver].add(-passed).at[sink].add(passed)
    labels = jnp.searchsorted(jnp.cumsum(lengths), jnp.arange(rows * top), side="right").astype(jnp.int32)
    grid = labels.reshape(top, rows).T
    grid = grid[jax.random.permutation(jax.random.fold_in(own, 1), rows)]
    offset_by = jax.random.randint(jax.random.fold_in(own, 2), (rows, 1), 0, top)
    return jnp.take_along_axis(grid, (jnp.arange(top)[None, :] + offset_by) % top, axis=1)


def shares(number_of, total, most, skew, full):
    weights = [(1 << 20) // math.isqrt(grade ** skew) + 1 for grade in range(1, number_of + 1)]
    largest = most if full else min(most, max(-(-total // number_of), total * weights[0] // sum(weights)))
    least = 1 if total - largest >= number_of - 1 else 0
    holding, rest = [largest] + [least] * (number_of - 1), total - largest - least * (number_of - 1)
    while rest > 0:
        candidates = [i for i in range(1, number_of) if holding[i] < largest] or [i for i in range(1, number_of) if holding[i] < most]
        pool, remaining = sum([weights[i] for i in candidates]), rest
        for i in candidates:
            extra = min(most - holding[i], max(1, remaining * weights[i] // pool), rest)
            holding[i] = holding[i] + extra
            rest = rest - extra
    return np.array(holding)


def gaussian(stream_key, shape, deviation, limit, split=(), kind=jnp.bfloat16):
    drawn = deviation * jax.random.normal(stream_key, shape, jnp.float32)
    if split:
        drawn = drawn * shard_levels(stream_key, shape, split, -0.22, 0.18)
    return jnp.clip(drawn, -limit, limit).astype(kind)


def setup_inputs(seed: int = 0) -> dict:
    streams_of = jax.random.split(jax.random.key(seed), 13)
    c_gate = gaussian(streams_of[0], (TOKA, WC), 1.0, 6.0, ((0, 8), (1, 4)))
    b_gate = gaussian(streams_of[1], (TOKA, WC), 1.0, 6.0, ((0, 8), (1, 4)))
    values = gaussian(streams_of[2], (TOKA, WC), 1.0, 6.0, ((0, 8), (1, 4)))
    conv_taps = gaussian(streams_of[3], (KCONV, WC), KCONV ** -0.5, 3.5, ((1, 4),), jnp.float32)
    w_mix_out = gaussian(streams_of[4], (WC, D), WC ** -0.5, 0.1875, ((0, 4),))
    moe_in = gaussian(streams_of[5], (TOKB, D), 1.0, 6.0, ((0, 32),))
    norm_gain = jnp.clip(1.0 + 0.18 * jax.random.normal(streams_of[6], (D,), jnp.float32), 0.1, 1.9)
    route_ids_keys = jax.random.split(jax.random.fold_in(streams_of[7], 1), TOKB // ROWS_B)
    route_ids_turns = jax.random.permutation(jax.random.fold_in(streams_of[7], 3), TOKB // ROWS_B)
    route_ids = jax.vmap(lambda own, number: shared_out(jax.random.fold_in(streams_of[7], 2), own, number, ROWS_B, EXPERTS, TOP, CAP, 1))(route_ids_keys, route_ids_turns).reshape((TOKB, TOP))
    route_weights = jnp.clip(0.1 + 0.9 * jax.random.uniform(streams_of[8], (TOKB, TOP), jnp.float32) ** shard_levels(streams_of[8], (TOKB, TOP), ((0, 32),), -0.2, 0.2), 0.1, 1.0)
    w_gate = gaussian(streams_of[9], (EXPERTS, D, FF), D ** -0.5, 0.125, ((0, 8), (2, 4)))
    w_up = gaussian(streams_of[10], (EXPERTS, D, FF), D ** -0.5, 0.125, ((0, 8), (2, 4)))
    w_down = gaussian(streams_of[11], (EXPERTS, FF, D), FF ** -0.5, 0.09375, ((0, 8), (1, 4)))
    return {"c_gate": c_gate, "b_gate": b_gate, "values": values, "conv_taps": conv_taps, "w_mix_out": w_mix_out, "moe_in": moe_in, "norm_gain": norm_gain, "route_ids": route_ids, "route_weights": route_weights, "w_gate": w_gate, "w_up": w_up, "w_down": w_down}


EPS = 1e-06

def grouped_product(left, right, groups):
    rows = left.shape[0]
    width = left.shape[1] // groups
    left_groups = left.reshape(rows, groups, width)
    right_groups = right.reshape(groups, width, right.shape[1])
    total = jnp.zeros((rows, right.shape[1]), jnp.float32)
    for group in range(groups):
        partial_value = jnp.dot(left_groups[:, group], right_groups[group], preferred_element_type=jnp.float32).astype(jnp.bfloat16)
        partial_value = lax.optimization_barrier(partial_value)
        total = total + partial_value.astype(jnp.float32)
    return total.astype(jnp.bfloat16)

def reference(c_gate, b_gate, values, conv_taps, w_mix_out, moe_in, norm_gain, route_ids, route_weights, w_gate, w_up, w_down):
    product = c_gate.astype(jnp.float32) * values.astype(jnp.float32)
    extended = jnp.concatenate([jnp.zeros((KCONV - 1, WC), jnp.float32), product], 0)
    convolved = jnp.zeros((TOKA, WC), jnp.float32)
    for offset in range(KCONV):
        convolved = convolved + conv_taps[offset][None, :] * extended[offset:offset + TOKA]
    mixed = (b_gate.astype(jnp.float32) * convolved).astype(jnp.bfloat16)
    mixer_out = grouped_product(mixed, w_mix_out, N_TP)
    stream = moe_in.astype(jnp.float32)
    scale = lax.rsqrt(lax.optimization_barrier(jnp.mean(stream * stream, axis=1, keepdims=True)) + EPS)
    normed = (stream * scale * norm_gain[None, :]).astype(jnp.bfloat16)
    copies = TOKB * TOP
    sources = N_EP * N_TP
    flat_ids = route_ids.reshape(sources, ROWS_B * TOP)
    onehot = (flat_ids[:, :, None] == jnp.arange(EXPERTS, dtype=jnp.int32)[None, None, :]).astype(jnp.int32)
    before = jnp.cumsum(onehot, axis=1) - onehot
    ranks_in = lax.optimization_barrier(jnp.sum(before * onehot, axis=2))
    slot_of = jnp.arange(sources, dtype=jnp.int32)[:, None] * CAP + ranks_in
    table = jnp.full((EXPERTS, SLOTS), copies, jnp.int32)
    table = table.at[flat_ids.reshape(-1), slot_of.reshape(-1)].set(jnp.arange(copies, dtype=jnp.int32))
    padded_rows = jnp.concatenate([normed, jnp.zeros((1, D), jnp.bfloat16)], 0)
    padded_weights = jnp.concatenate([route_weights.reshape(-1), jnp.zeros((1,), jnp.float32)], 0)

    def per_expert(carry, inputs):
        expert_table, gate_mat, up_mat, down_mat = inputs
        row_index = expert_table // TOP
        rows = padded_rows[row_index]
        gate_val = jnp.dot(rows, gate_mat, preferred_element_type=jnp.float32)
        up_val = jnp.dot(rows, up_mat, preferred_element_type=jnp.float32)
        hidden = (jax.nn.silu(gate_val) * up_val).astype(jnp.bfloat16)
        expert_out = grouped_product(hidden, down_mat, N_TP)
        weighted = expert_out.astype(jnp.float32) * padded_weights[expert_table][:, None]
        carry = carry.at[row_index].add(weighted, mode='drop')
        return (carry, None)
    summed, unused = lax.scan(per_expert, jnp.zeros((TOKB, D), jnp.float32), (table, w_gate, w_up, w_down))
    moe_out = summed.astype(jnp.bfloat16)
    return (mixer_out, moe_out)
```

```python
import functools

import jax
import jax.numpy as jnp
from jax import lax
from jax.experimental import pallas as pl
from jax.experimental.pallas import tpu as pltpu
from jax.sharding import PartitionSpec as P

EPS = 1e-06
PAIRS = 4
MESH = pl.DeviceIdType.MESH


def passed_along(block, axis, distance):
    devices = range(lax.axis_size(axis))
    route = [(i - distance, i) for i in devices if i - distance in devices]
    return lax.ppermute(block, axis, route)


def remote(src, dst, send_sem, recv_sem, ep, tp):
    return pltpu.make_async_remote_copy(
        src_ref=src,
        dst_ref=dst,
        send_sem=send_sem,
        recv_sem=recv_sem,
        device_id=(ep, tp),
        device_id_type=MESH,
    )


def places():
    ep = lax.axis_index("ep")
    tp = lax.axis_index("tp")
    partner = tp + 1 - 2 * (tp % 2)
    across = (tp + 2) % PAIRS
    diagonal = (partner + 2) % PAIRS
    return ep, tp, partner, across, diagonal


def greet(n, ep, tp, partner, across):
    barrier = pltpu.get_barrier_semaphore()

    def hello(s, carry):
        pl.semaphore_signal(
            barrier, inc=1, device_id=((ep + s) % n, tp), device_id_type=MESH
        )
        return carry

    lax.fori_loop(1, n, hello, 0)
    pl.semaphore_signal(barrier, inc=1, device_id=(ep, partner), device_id_type=MESH)
    pl.semaphore_signal(barrier, inc=1, device_id=(ep, across), device_id_type=MESH)
    pl.semaphore_wait(barrier, n + 1)


def loop(lower, upper, body):
    lax.fori_loop(lower, upper, lambda s, carry: (body(s), carry)[1], 0)


def dispatch_kernel(
    n, own, all_rows, a_send, a_recv, c_send, c_recv, x_send, x_recv, r_send, r_recv, local_sem
):
    ep, tp, partner, across, diagonal = places()
    local = pltpu.make_async_copy(own.at[ep], all_rows.at[tp, ep], local_sem)
    local.start()
    greet(n, ep, tp, partner, across)

    def to_expert(s):
        to = (ep + s) % n
        return remote(own.at[to], all_rows.at[tp, ep], a_send.at[s], a_recv.at[s], to, tp)

    def from_source(s):
        to = (ep + s) % n
        return remote(
            own.at[to], all_rows.at[tp, (ep + n - s) % n], a_send.at[s], a_recv.at[s], to, tp
        )

    def shared(s, row, sends, recvs, to):
        block = all_rows.at[row, (ep + n - s) % n]
        return remote(block, block, sends.at[s], recvs.at[s], ep, to)

    loop(1, n, lambda s: to_expert(s).start())
    local.wait()

    def share(s):
        shared(s, tp, x_send, x_recv, across).start()
        shared(s, tp, c_send, c_recv, partner).start()

    share(0)

    def arrive(s):
        from_source(s).wait_recv()
        share(s)

    loop(1, n, arrive)

    def relay(s):
        shared(s, across, x_send, x_recv, across).wait_recv()
        shared(s, across, r_send, r_recv, partner).start()

    loop(0, n, relay)

    def finish(s):
        shared(s, tp, x_send, x_recv, across).wait_send()
        shared(s, tp, c_send, c_recv, partner).wait_send()
        shared(s, partner, c_send, c_recv, partner).wait_recv()
        shared(s, across, r_send, r_recv, partner).wait_send()
        shared(s, diagonal, r_send, r_recv, partner).wait_recv()

    loop(0, n, finish)
    loop(1, n, lambda s: to_expert(s).wait_send())


def added(*blocks):
    total = blocks[0].astype(jnp.float32)
    for block in blocks[1:]:
        total = total + block.astype(jnp.float32)
    return total.astype(jnp.bfloat16)


def combine_kernel(
    n,
    parts,
    mix_parts,
    back,
    mix_out,
    c_in,
    x_out,
    x_in,
    done,
    mc_in,
    mx_out,
    mx_in,
    c_send,
    c_recv,
    d_send,
    d_recv,
    x_send,
    x_recv,
    a_send,
    a_recv,
    m_send,
    m_recv,
):
    ep, tp, partner, across, diagonal = places()
    greet(n, ep, tp, partner, across)

    def to_of(s):
        return (ep + 1 + s) % n

    def far(s):
        return remote(
            parts.at[diagonal, to_of(s)], c_in.at[1, s], d_send.at[s], d_recv.at[s], ep, partner
        )

    def near(s):
        return remote(
            parts.at[partner, to_of(s)], c_in.at[0, s], c_send.at[s], c_recv.at[s], ep, partner
        )

    def cross(s):
        return remote(x_out.at[s], x_in.at[s], x_send.at[s], x_recv.at[s], ep, across)

    def home(s):
        return remote(done.at[s], back.at[ep], a_send.at[s], a_recv.at[s], to_of(s), tp)

    def home_arrived(s):
        return remote(
            done.at[s],
            back.at[(ep + n - 1 - s) % n],
            a_send.at[s],
            a_recv.at[s],
            to_of(s),
            tp,
        )

    m_far = remote(mix_parts.at[diagonal], mc_in.at[1], m_send.at[0], m_recv.at[0], ep, partner)
    m_near = remote(mix_parts.at[partner], mc_in.at[0], m_send.at[1], m_recv.at[1], ep, partner)
    m_cross = remote(mx_out, mx_in, m_send.at[2], m_recv.at[2], ep, across)

    loop(0, n, lambda s: far(s).start())
    m_far.start()
    loop(0, n, lambda s: near(s).start())
    m_near.start()

    def first_sum(s):
        far(s).wait_recv()
        x_out[s] = added(parts[across, to_of(s)], c_in[1, s])
        cross(s).start()

    loop(0, n, first_sum)
    m_far.wait_recv()
    mx_out[...] = added(mix_parts[across], mc_in[1])
    m_cross.start()

    def second_sum(s):
        near(s).wait_recv()
        cross(s).wait_recv()
        return added(parts[tp, to_of(s)], c_in[0, s], x_in[s])

    def send_home(s):
        done[s] = second_sum(s)
        home(s).start()

    loop(0, n - 1, send_home)
    back[ep] = second_sum(n - 1)
    m_near.wait_recv()
    m_cross.wait_recv()
    mix_out[...] = added(mix_parts[tp], mc_in[0], mx_in[...])

    def finish(s):
        far(s).wait_send()
        near(s).wait_send()
        cross(s).wait_send()

    loop(0, n, finish)

    def finish_home(s):
        home_arrived(s).wait_recv()
        home(s).wait_send()

    loop(0, n - 1, finish_home)
    m_far.wait_send()
    m_near.wait_send()
    m_cross.wait_send()


def dispatch(own, n):
    sems = [pltpu.SemaphoreType.DMA((n,))] * 8 + [pltpu.SemaphoreType.DMA]
    return pl.pallas_call(
        functools.partial(dispatch_kernel, n),
        out_shape=jax.ShapeDtypeStruct((PAIRS,) + own.shape, own.dtype),
        in_specs=[pl.BlockSpec(memory_space=pltpu.VMEM)],
        out_specs=pl.BlockSpec(memory_space=pl.ANY),
        scratch_shapes=sems,
        compiler_params=pltpu.CompilerParams(collective_id=0, has_side_effects=True),
        cost_estimate=pl.CostEstimate(
            flops=30_000_000_000, bytes_accessed=10_000_000, transcendentals=0
        ),
        name="dispatch",
    )(own)


def combine(parts, mix_parts, n):
    block = parts.shape[2:]
    mix_block = mix_parts.shape[1:]
    kind = parts.dtype
    vmem = pl.BlockSpec(memory_space=pltpu.VMEM)
    return pl.pallas_call(
        functools.partial(combine_kernel, n),
        out_shape=(
            jax.ShapeDtypeStruct((n,) + block, kind),
            jax.ShapeDtypeStruct(mix_block, kind),
        ),
        in_specs=[vmem, vmem],
        out_specs=(vmem, vmem),
        scratch_shapes=[
            pltpu.VMEM((2, n) + block, kind),
            pltpu.VMEM((n,) + block, kind),
            pltpu.VMEM((n,) + block, kind),
            pltpu.VMEM((n,) + block, kind),
            pltpu.VMEM((2,) + mix_block, kind),
            pltpu.VMEM(mix_block, kind),
            pltpu.VMEM(mix_block, kind),
        ]
        + [pltpu.SemaphoreType.DMA((n,))] * 8
        + [pltpu.SemaphoreType.DMA((3,))] * 2,
        compiler_params=pltpu.CompilerParams(collective_id=1, has_side_effects=True),
        name="combine",
    )(parts, mix_parts)


def on_device(
    c_gate,
    b_gate,
    values,
    conv_taps,
    w_mix_out,
    moe_in,
    norm_gain,
    route_ids,
    route_weights,
    w_gate,
    w_up,
    w_down,
):
    n_tp = lax.axis_size("tp")
    assert n_tp == PAIRS
    tokens = c_gate.shape[0]
    reach = conv_taps.shape[0] - 1
    product = c_gate.astype(jnp.float32) * values.astype(jnp.float32)
    previous = passed_along(product[tokens - reach :], "ep", 1)
    extended = jnp.concatenate([previous, product], 0)
    convolved = jnp.zeros_like(product)
    for offset in range(reach + 1):
        convolved = convolved + conv_taps[offset][None, :] * extended[offset : offset + tokens]
    mixed = (b_gate.astype(jnp.float32) * convolved).astype(jnp.bfloat16)
    mix_parts = jnp.dot(mixed, w_mix_out, preferred_element_type=jnp.float32).astype(jnp.bfloat16)
    mix_parts = mix_parts.reshape(n_tp, tokens // n_tp, -1)

    rows_b = moe_in.shape[0]
    width = moe_in.shape[1]
    top = route_ids.shape[1]
    n_ep = lax.axis_size("ep")
    experts = w_gate.shape[0] * n_ep
    capacity = 5 * rows_b * top // (4 * experts)
    stream = moe_in.astype(jnp.float32)
    scale = lax.rsqrt(jnp.mean(stream * stream, axis=1, keepdims=True) + EPS)
    normed = (stream * scale * norm_gain[None, :]).astype(jnp.bfloat16)

    expert_at = jnp.arange(experts, dtype=jnp.int32)[:, None]
    chosen = jnp.zeros((experts, rows_b), jnp.bool_)
    weight = jnp.zeros((experts, rows_b), jnp.float32)
    for j in range(top):
        match = route_ids[:, j][None, :] == expert_at
        chosen = chosen | match
        weight = weight + jnp.where(match, route_weights[:, j][None, :], 0.0)
    token_at = jnp.arange(rows_b, dtype=jnp.int32)
    earlier = (token_at[:, None] < token_at[None, :]).astype(jnp.bfloat16)
    rank = jnp.dot(
        chosen.astype(jnp.bfloat16), earlier, preferred_element_type=jnp.float32
    ).astype(jnp.int32)
    slot_at = jnp.arange(capacity, dtype=jnp.int32)[None, :, None]
    placed = (rank[:, None, :] == slot_at) & chosen[:, None, :]
    select = placed.astype(jnp.bfloat16).reshape(experts * capacity, rows_b)
    own = jnp.dot(select, normed, preferred_element_type=jnp.float32).astype(jnp.bfloat16)

    piece = dispatch(own.reshape(experts, capacity, width), n_ep).reshape(-1, width)
    gate_val = jnp.dot(piece, w_gate[0], preferred_element_type=jnp.float32)
    up_val = jnp.dot(piece, w_up[0], preferred_element_type=jnp.float32)
    hidden = (jax.nn.silu(gate_val) * up_val).astype(jnp.bfloat16)
    parts = jnp.dot(hidden, w_down[0], preferred_element_type=jnp.float32).astype(jnp.bfloat16)
    returned, mixer_out = combine(
        parts.reshape(n_tp, n_ep, capacity, width), mix_parts, n_ep
    )
    returned = returned.reshape(-1, width)

    spread = jnp.where(placed, weight[:, None, :], 0.0).reshape(experts * capacity, rows_b)
    high = lax.reduce_precision(spread, 8, 7)
    low = (spread - high).astype(jnp.bfloat16)
    over_slots = (((0,), (0,)), ((), ()))
    moe_out = lax.dot_general(
        high.astype(jnp.bfloat16), returned, over_slots, preferred_element_type=jnp.float32
    ) + lax.dot_general(low, returned, over_slots, preferred_element_type=jnp.float32)
    return (mixer_out, moe_out.astype(jnp.bfloat16))


def solution(mesh):
    return jax.shard_map(
        on_device,
        mesh=mesh,
        in_specs=(
            P("ep", "tp"),
            P("ep", "tp"),
            P("ep", "tp"),
            P(None, "tp"),
            P("tp", None),
            P(("ep", "tp"), None),
            P(),
            P(("ep", "tp"), None),
            P(("ep", "tp"), None),
            P("ep", None, "tp"),
            P("ep", None, "tp"),
            P("ep", "tp", None),
        ),
        out_specs=(P(("ep", "tp"), None), P(("ep", "tp"), None)),
        check_vma=False,
    )
```

```python
import functools

import jax
import jax.numpy as jnp
from jax import lax
from jax.experimental import pallas as pl
from jax.experimental.pallas import tpu as pltpu
from jax.sharding import PartitionSpec as P

EPS = 1e-06
PAIRS = 4
MESH = pl.DeviceIdType.MESH


def remote(src, dst, send_sem, recv_sem, ep, tp):
    return pltpu.make_async_remote_copy(
        src_ref=src,
        dst_ref=dst,
        send_sem=send_sem,
        recv_sem=recv_sem,
        device_id=(ep, tp),
        device_id_type=MESH,
    )


def places():
    ep = lax.axis_index("ep")
    tp = lax.axis_index("tp")
    partner = tp + 1 - 2 * (tp % 2)
    across = (tp + 2) % PAIRS
    diagonal = (partner + 2) % PAIRS
    return ep, tp, partner, across, diagonal


def greet(n, ep, tp, partner, across):
    barrier = pltpu.get_barrier_semaphore()

    def hello(s, carry):
        pl.semaphore_signal(
            barrier, inc=1, device_id=((ep + s) % n, tp), device_id_type=MESH
        )
        return carry

    lax.fori_loop(1, n, hello, 0)
    pl.semaphore_signal(barrier, inc=1, device_id=(ep, partner), device_id_type=MESH)
    pl.semaphore_signal(barrier, inc=1, device_id=(ep, across), device_id_type=MESH)
    pl.semaphore_wait(barrier, n + 1)


def loop(lower, upper, body):
    lax.fori_loop(lower, upper, lambda s, carry: (body(s), carry)[1], 0)


def dispatch_kernel(
    n,
    own,
    tail,
    all_rows,
    previous,
    a_send,
    a_recv,
    c_send,
    c_recv,
    x_send,
    x_recv,
    r_send,
    r_recv,
    local_sem,
    t_send,
    t_recv,
):
    ep, tp, partner, across, diagonal = places()
    local = pltpu.make_async_copy(own.at[ep], all_rows.at[tp, ep], local_sem)
    local.start()
    greet(n, ep, tp, partner, across)
    onward = remote(tail, previous, t_send, t_recv, (ep + 1) % n, tp)
    onward.start()

    def to_expert(s):
        to = (ep + s) % n
        return remote(own.at[to], all_rows.at[tp, ep], a_send.at[s], a_recv.at[s], to, tp)

    def from_source(s):
        to = (ep + s) % n
        return remote(
            own.at[to], all_rows.at[tp, (ep + n - s) % n], a_send.at[s], a_recv.at[s], to, tp
        )

    def shared(s, row, sends, recvs, to):
        block = all_rows.at[row, (ep + n - s) % n]
        return remote(block, block, sends.at[s], recvs.at[s], ep, to)

    loop(1, n, lambda s: to_expert(s).start())
    local.wait()

    def share(s):
        shared(s, tp, x_send, x_recv, across).start()
        shared(s, tp, c_send, c_recv, partner).start()

    share(0)

    def arrive(s):
        from_source(s).wait_recv()
        share(s)

    def relay(s):
        shared(s, across, x_send, x_recv, across).wait_recv()
        shared(s, across, r_send, r_recv, partner).start()

    lag = min(3, n - 1)

    def arrive_and_relay(s):
        arrive(s)
        relay(s - lag)

    loop(1, lag, arrive)
    loop(lag, n, arrive_and_relay)
    loop(n - lag, n, relay)

    def finish(s):
        shared(s, tp, x_send, x_recv, across).wait_send()
        shared(s, tp, c_send, c_recv, partner).wait_send()
        shared(s, partner, c_send, c_recv, partner).wait_recv()
        shared(s, across, r_send, r_recv, partner).wait_send()
        shared(s, diagonal, r_send, r_recv, partner).wait_recv()

    loop(0, n, finish)
    loop(1, n, lambda s: to_expert(s).wait_send())
    onward.wait()


def added(*blocks):
    total = blocks[0].astype(jnp.float32)
    for block in blocks[1:]:
        total = total + block.astype(jnp.float32)
    return total.astype(jnp.bfloat16)


def combine_kernel(
    n,
    parts,
    mix_parts,
    back,
    mix_out,
    c_in,
    x_out,
    x_in,
    done,
    mc_in,
    mx_out,
    mx_in,
    c_send,
    c_recv,
    d_send,
    d_recv,
    x_send,
    x_recv,
    a_send,
    a_recv,
    m_send,
    m_recv,
):
    ep, tp, partner, across, diagonal = places()
    greet(n, ep, tp, partner, across)

    def to_of(s):
        return (ep + 1 + s) % n

    def far(s):
        return remote(
            parts.at[diagonal, to_of(s)], c_in.at[1, s], d_send.at[s], d_recv.at[s], ep, partner
        )

    def near(s):
        return remote(
            parts.at[partner, to_of(s)], c_in.at[0, s], c_send.at[s], c_recv.at[s], ep, partner
        )

    def cross(s):
        return remote(x_out.at[s], x_in.at[s], x_send.at[s], x_recv.at[s], ep, across)

    def home(s):
        return remote(done.at[s], back.at[ep], a_send.at[s], a_recv.at[s], to_of(s), tp)

    def home_arrived(s):
        return remote(
            done.at[s],
            back.at[(ep + n - 1 - s) % n],
            a_send.at[s],
            a_recv.at[s],
            to_of(s),
            tp,
        )

    m_far = remote(mix_parts.at[diagonal], mc_in.at[1], m_send.at[0], m_recv.at[0], ep, partner)
    m_near = remote(mix_parts.at[partner], mc_in.at[0], m_send.at[1], m_recv.at[1], ep, partner)
    m_cross = remote(mx_out, mx_in, m_send.at[2], m_recv.at[2], ep, across)

    loop(0, n, lambda s: far(s).start())
    m_far.start()
    loop(0, n, lambda s: near(s).start())
    m_near.start()

    def first_sum(s):
        far(s).wait_recv()
        x_out[s] = added(parts[across, to_of(s)], c_in[1, s])
        cross(s).start()

    loop(0, n, first_sum)
    m_far.wait_recv()
    mx_out[...] = added(mix_parts[across], mc_in[1])
    m_cross.start()

    def second_sum(s):
        near(s).wait_recv()
        cross(s).wait_recv()
        return added(parts[tp, to_of(s)], c_in[0, s], x_in[s])

    def send_home(s):
        done[s] = second_sum(s)
        home(s).start()

    loop(0, n - 1, send_home)
    back[ep] = second_sum(n - 1)
    m_near.wait_recv()
    m_cross.wait_recv()
    mix_out[...] = added(mix_parts[tp], mc_in[0], mx_in[...])

    def finish(s):
        far(s).wait_send()
        near(s).wait_send()
        cross(s).wait_send()

    loop(0, n, finish)

    def finish_home(s):
        home_arrived(s).wait_recv()
        home(s).wait_send()

    loop(0, n - 1, finish_home)
    m_far.wait_send()
    m_near.wait_send()
    m_cross.wait_send()


def dispatch(own, tail, n):
    sems = [pltpu.SemaphoreType.DMA((n,))] * 8 + [pltpu.SemaphoreType.DMA] * 3
    vmem = pl.BlockSpec(memory_space=pltpu.VMEM)
    return pl.pallas_call(
        functools.partial(dispatch_kernel, n),
        out_shape=(
            jax.ShapeDtypeStruct((PAIRS,) + own.shape, own.dtype),
            jax.ShapeDtypeStruct(tail.shape, tail.dtype),
        ),
        in_specs=[vmem, vmem],
        out_specs=(pl.BlockSpec(memory_space=pl.ANY), vmem),
        scratch_shapes=sems,
        compiler_params=pltpu.CompilerParams(collective_id=0, has_side_effects=True),
        cost_estimate=pl.CostEstimate(
            flops=30_000_000_000, bytes_accessed=10_000_000, transcendentals=0
        ),
        name="dispatch",
    )(own, tail)


def combine(parts, mix_parts, n):
    block = parts.shape[2:]
    mix_block = mix_parts.shape[1:]
    kind = parts.dtype
    vmem = pl.BlockSpec(memory_space=pltpu.VMEM)
    return pl.pallas_call(
        functools.partial(combine_kernel, n),
        out_shape=(
            jax.ShapeDtypeStruct((n,) + block, kind),
            jax.ShapeDtypeStruct(mix_block, kind),
        ),
        in_specs=[vmem, vmem],
        out_specs=(vmem, vmem),
        scratch_shapes=[
            pltpu.VMEM((2, n) + block, kind),
            pltpu.VMEM((n,) + block, kind),
            pltpu.VMEM((n,) + block, kind),
            pltpu.VMEM((n,) + block, kind),
            pltpu.VMEM((2,) + mix_block, kind),
            pltpu.VMEM(mix_block, kind),
            pltpu.VMEM(mix_block, kind),
        ]
        + [pltpu.SemaphoreType.DMA((n,))] * 8
        + [pltpu.SemaphoreType.DMA((3,))] * 2,
        compiler_params=pltpu.CompilerParams(collective_id=1, has_side_effects=True),
        name="combine",
    )(parts, mix_parts)


def on_device(
    c_gate,
    b_gate,
    values,
    conv_taps,
    w_mix_out,
    moe_in,
    norm_gain,
    route_ids,
    route_weights,
    w_gate,
    w_up,
    w_down,
):
    n_tp = lax.axis_size("tp")
    assert n_tp == PAIRS
    tokens = c_gate.shape[0]
    reach = conv_taps.shape[0] - 1
    product = c_gate.astype(jnp.float32) * values.astype(jnp.float32)
    rows_b = moe_in.shape[0]
    width = moe_in.shape[1]
    top = route_ids.shape[1]
    n_ep = lax.axis_size("ep")
    experts = w_gate.shape[0] * n_ep
    capacity = 5 * rows_b * top // (4 * experts)
    stream = moe_in.astype(jnp.float32)
    scale = lax.rsqrt(jnp.mean(stream * stream, axis=1, keepdims=True) + EPS)
    normed = (stream * scale * norm_gain[None, :]).astype(jnp.bfloat16)

    expert_at = jnp.arange(experts, dtype=jnp.int32)[:, None]
    chosen = jnp.zeros((experts, rows_b), jnp.bool_)
    weight = jnp.zeros((experts, rows_b), jnp.float32)
    for j in range(top):
        match = route_ids[:, j][None, :] == expert_at
        chosen = chosen | match
        weight = weight + jnp.where(match, route_weights[:, j][None, :], 0.0)
    token_at = jnp.arange(rows_b, dtype=jnp.int32)
    earlier = (token_at[:, None] < token_at[None, :]).astype(jnp.bfloat16)
    rank = jnp.dot(
        chosen.astype(jnp.bfloat16), earlier, preferred_element_type=jnp.float32
    ).astype(jnp.int32)
    slot_at = jnp.arange(capacity, dtype=jnp.int32)[None, :, None]
    placed = (rank[:, None, :] == slot_at) & chosen[:, None, :]
    select = placed.astype(jnp.bfloat16).reshape(experts * capacity, rows_b)
    own = jnp.dot(select, normed, preferred_element_type=jnp.float32).astype(jnp.bfloat16)

    arrived, previous = dispatch(
        own.reshape(experts, capacity, width), product[tokens - reach :], n_ep
    )
    piece = arrived.reshape(-1, width)
    previous = jnp.where(lax.axis_index("ep") == 0, 0.0, previous)
    extended = jnp.concatenate([previous, product], 0)
    convolved = jnp.zeros_like(product)
    for offset in range(reach + 1):
        convolved = convolved + conv_taps[offset][None, :] * extended[offset : offset + tokens]
    mixed = (b_gate.astype(jnp.float32) * convolved).astype(jnp.bfloat16)
    mix_parts = jnp.dot(mixed, w_mix_out, preferred_element_type=jnp.float32).astype(jnp.bfloat16)
    mix_parts = mix_parts.reshape(n_tp, tokens // n_tp, -1)
    gate_val = jnp.dot(piece, w_gate[0], preferred_element_type=jnp.float32)
    up_val = jnp.dot(piece, w_up[0], preferred_element_type=jnp.float32)
    hidden = (jax.nn.silu(gate_val) * up_val).astype(jnp.bfloat16)
    parts = jnp.dot(hidden, w_down[0], preferred_element_type=jnp.float32).astype(jnp.bfloat16)
    returned, mixer_out = combine(
        parts.reshape(n_tp, n_ep, capacity, width), mix_parts, n_ep
    )
    returned = returned.reshape(-1, width)

    spread = jnp.where(placed, weight[:, None, :], 0.0).reshape(experts * capacity, rows_b)
    high = lax.reduce_precision(spread, 8, 7)
    low = (spread - high).astype(jnp.bfloat16)
    over_slots = (((0,), (0,)), ((), ()))
    moe_out = lax.dot_general(
        high.astype(jnp.bfloat16), returned, over_slots, preferred_element_type=jnp.float32
    ) + lax.dot_general(low, returned, over_slots, preferred_element_type=jnp.float32)
    return (mixer_out, moe_out.astype(jnp.bfloat16))


def solution(mesh):
    return jax.shard_map(
        on_device,
        mesh=mesh,
        in_specs=(
            P("ep", "tp"),
            P("ep", "tp"),
            P("ep", "tp"),
            P(None, "tp"),
            P("tp", None),
            P(("ep", "tp"), None),
            P(),
            P(("ep", "tp"), None),
            P(("ep", "tp"), None),
            P("ep", None, "tp"),
            P("ep", None, "tp"),
            P("ep", "tp", None),
        ),
        out_specs=(P(("ep", "tp"), None), P(("ep", "tp"), None)),
        check_vma=False,
    )
```
